1024 devices in a mesh: ep: 64 (over z, core), tp: 16 (over y, x).
Axes of the slice: x: 4, y: 4, z: 32, core: 2. Of those that a mesh axis runs over, the one named last changes fastest.
Arguments:
- tokens: bfloat16 [16384, 2048], P('ep'), may hold values from -6 to 6
- norm_gain: float32 [2048], replicated, may hold values from 0.1 to 1.9
- route_ids: int32 [16384, 4], P('ep'), may hold values from 0 to 127, all different within a row; in each aligned block of 256 rows (0 to 255, 256 to 511, ...) at most 12 rows name the same one
- route_weights: float32 [16384, 4], P('ep'), may hold values from 0.1 to 1
- w_gate: bfloat16 [128, 2048, 2048], P('ep', None, 'tp'), may hold values from -0.33007812 to 0.33007812
- w_up: bfloat16 [128, 2048, 2048], P('ep', None, 'tp'), may hold values from -0.33007812 to 0.33007812
- w_down: bfloat16 [128, 2048, 2048], P('ep', None, 'tp'), may hold values from -0.026489258 to 0.026489258
Outputs:
- mixed_out: bfloat16 [16384, 2048], P('ep', 'tp')
The draws below stay inside these ranges and needn't reach their ends.
Inputs may be any that keep to these rules, and one draw needn't show every extreme that they name: `route_ids`: each token names 4 different experts. Within the tokens of one index of ep (aligned blocks of 256 tokens) no expert is named more than 12 times, a bound that some block reaches.
All inputs are finite; a program needn't handle non-finite values.
Results may differ from the reference program's by a relative error of at most 0.007.
Values may be sent and summed in bfloat16 or wider, within the bound.
No kernel may reach another device: no remote copies, remote signals or barrier semaphores. Data moves between devices by JAX's collectives and lax.ppermute only.
A program may use at most 32 MiB of HBM per device.

```python
import math
import jax
import jax.numpy as jnp
import numpy as np
from jax import lax

D = 2048
FF = 2048
TOP_K = 4
TOK_DEV = 256
EXPERTS = 128
TOKENS = 16384
CAP = 12
N_EP = 64


def block_scale(rng, shape, split, smallest, top_value):
    def one(axis_at, parts):
        heights = jax.random.uniform(jax.random.fold_in(jax.random.fold_in(rng, 6), axis_at), (parts,), jnp.float32, smallest / len(split), top_value / len(split))
        return jnp.repeat(jnp.exp(heights), shape[axis_at] // parts).reshape((-1,) + (1,) * (len(shape) - axis_at - 1))

    level = one(*split[0])
    for cut in split[1:]:
        level = level * one(*cut)
    return level


def assign_block(own_key, own, number, rows, amount, top, reach, lean):
    ranking = jax.random.permutation(own_key, amount)
    crowded, ordinary = load_shares(amount, rows * top, reach, lean, True), load_shares(amount, rows * top, reach, lean, False)
    places = jnp.arange(amount)

    def named(tallies, offset_by):
        used = int((tallies > 0).sum())
        fixed = max(1, used // 4)
        passed = fixed + (places - fixed + offset_by * (used - fixed)) % max(1, amount - fixed)
        return jnp.zeros((amount,), jnp.int32).at[ranking[jnp.where(places < fixed, places, passed)]].set(jnp.asarray(tallies, jnp.int32))

    tallies = jnp.where(number % 4 == 0, named(crowded, number // 4), named(ordinary, number - number // 4 - 1))
    mixed = jax.random.permutation(jax.random.fold_in(own, 3), amount)
    giver, sink = mixed[0:amount // 2 * 2:2], mixed[1:amount // 2 * 2:2]
    room = jnp.minimum(tallies[giver] - 1, reach - tallies[sink]) // 2
    room = jnp.where((giver == ranking[0]) | (sink == ranking[0]) | (tallies[sink] == 0), 0, jnp.maximum(room, 0))
    passed = jax.random.randint(jax.random.fold_in(own, 4), (amount // 2,), 0, 1 << 20) % (room + 1)
    tallies = tallies.at[giver].add(-passed).at[sink].add(passed)
    members = jnp.searchsorted(jnp.cumsum(tallies), jnp.arange(rows * top), side="right").astype(jnp.int32)
    listing = members.reshape(top, rows).T
    listing = listing[jax.random.permutation(jax.random.fold_in(own, 1), rows)]
    offset_by = jax.random.randint(jax.random.fold_in(own, 2), (rows, 1), 0, top)
    return jnp.take_along_axis(listing, (jnp.arange(top)[None, :] + offset_by) % top, axis=1)


def load_shares(number_of, total, reach, slope, full):
    portions = [(1 << 20) // math.isqrt(grade ** slope) + 1 for grade in range(1, number_of + 1)]
    largest = reach if full else min(reach, max(-(-total // number_of), total * portions[0] // sum(portions)))
    least = 1 if total - largest >= number_of - 1 else 0
    counts, spare = [largest] + [least] * (number_of - 1), total - largest - least * (number_of - 1)
    while spare > 0:
        free = [i for i in range(1, number_of) if counts[i] < largest] or [i for i in range(1, number_of) if counts[i] < reach]
        whole, remaining = sum([portions[i] for i in free]), spare
        for i in free:
            extra = min(reach - counts[i], max(1, remaining * portions[i] // whole), spare)
            counts[i] = counts[i] + extra
            spare = spare - extra
    return np.array(counts)


def scatter_about(own_key, extent, scale, limit, split=(), kind=jnp.bfloat16):
    entries = scale * jax.random.normal(own_key, extent, jnp.float32)
    if split:
        entries = entries * block_scale(own_key, extent, split, -0.22, 0.18)
    return jnp.clip(entries, -limit, limit).astype(kind)


def setup_inputs(seed: int = 0) -> dict:
    splits = jax.random.split(jax.random.key(seed), 8)
    tokens = scatter_about(splits[0], (TOKENS, D), 1.0, 6.0, ((0, 64),))
    norm_gain = jnp.clip(1.0 + 0.18 * jax.random.normal(splits[1], (D,), jnp.float32), 0.1, 1.9)
    route_ids_keys = jax.random.split(jax.random.fold_in(splits[2], 1), TOKENS // TOK_DEV)
    route_ids_turns = jax.random.permutation(jax.random.fold_in(splits[2], 3), TOKENS // TOK_DEV)
    route_ids = jax.vmap(lambda own, number: assign_block(jax.random.fold_in(splits[2], 2), own, number, TOK_DEV, EXPERTS, TOP_K, CAP, 2))(route_ids_keys, route_ids_turns).reshape((TOKENS, TOP_K))
    route_weights = jnp.clip(0.1 + 0.9 * jax.random.uniform(splits[3], (TOKENS, TOP_K), jnp.float32) ** block_scale(splits[3], (TOKENS, TOP_K), ((0, 64),), -0.2, 0.2), 0.1, 1.0)
    w_gate = scatter_about(splits[4], (EXPERTS, D, FF), (2.5 * D ** -0.5), 0.33007812, ((0, 64), (2, 16)))
    w_up = scatter_about(splits[5], (EXPERTS, D, FF), (2.5 * D ** -0.5), 0.33007812, ((0, 64), (2, 16)))
    w_down = scatter_about(splits[6], (EXPERTS, FF, D), (0.2 * FF ** -0.5), 0.026489258, ((0, 64), (2, 16)))
    return {"tokens": tokens, "norm_gain": norm_gain, "route_ids": route_ids, "route_weights": route_weights, "w_gate": w_gate, "w_up": w_up, "w_down": w_down}


swiglu_limit = 7.0
swiglu_alpha = 1.702
norm_eps = 1e-05

def clamped_units(gate_pre, up_pre):
    capped = jnp.minimum(gate_pre, swiglu_limit)
    linear = jnp.clip(up_pre, -swiglu_limit, swiglu_limit)
    return capped * jax.nn.sigmoid(swiglu_alpha * capped) * (linear + 1.0)

def slots_of(group_ids):
    matches = (group_ids[:, None] == jnp.arange(EXPERTS, dtype=jnp.int32)[None, :]).astype(jnp.int32)
    earlier = jnp.cumsum(matches, axis=0) - matches
    return lax.optimization_barrier(jnp.sum(earlier * matches, axis=1)).astype(jnp.int32)

def one_expert(args):
    row_block, gate_weight, up_weight, down_weight = args
    row_values = row_block.astype(jnp.float32)
    gate_pre = jnp.dot(row_values, gate_weight.astype(jnp.float32), preferred_element_type=jnp.float32)
    up_pre = jnp.dot(row_values, up_weight.astype(jnp.float32), preferred_element_type=jnp.float32)
    activation = clamped_units(gate_pre, up_pre).astype(jnp.bfloat16)
    result = jnp.dot(activation.astype(jnp.float32), down_weight.astype(jnp.float32), preferred_element_type=jnp.float32)
    return result.astype(jnp.bfloat16)

def reference(tokens, norm_gain, route_ids, route_weights, w_gate, w_up, w_down):
    values = tokens.astype(jnp.float32)
    row_mean = lax.optimization_barrier(jnp.mean(values, axis=1, keepdims=True))
    centred = values - row_mean
    row_var = lax.optimization_barrier(jnp.mean(centred * centred, axis=1, keepdims=True))
    normed = (centred * lax.rsqrt(row_var + norm_eps) * norm_gain).astype(jnp.bfloat16)
    group_ids = route_ids.reshape(N_EP, TOK_DEV * TOP_K).astype(jnp.int32)
    slot_index = lax.map(slots_of, group_ids)
    group_rank = jnp.arange(N_EP, dtype=jnp.int32)[:, None]
    position = (group_ids * (N_EP * CAP) + group_rank * CAP + slot_index).reshape(-1).astype(jnp.int32)
    source_rows = jnp.repeat(normed, TOP_K, axis=0)
    buffer = jnp.zeros((EXPERTS * N_EP * CAP, D), jnp.bfloat16).at[position].set(source_rows)
    results = lax.map(one_expert, (buffer.reshape(EXPERTS, N_EP * CAP, D), w_gate, w_up, w_down))
    picked = results.reshape(EXPERTS * N_EP * CAP, D)[position].reshape(TOKENS, TOP_K, D).astype(jnp.float32)
    return lax.optimization_barrier(jnp.sum(picked * route_weights[:, :, None], axis=1)).astype(jnp.bfloat16)
```

```python
import functools

import jax
import jax.numpy as jnp
import numpy as np
from jax import lax
from jax.experimental import pallas as pl
from jax.experimental.pallas import tpu as pltpu
from jax.sharding import PartitionSpec as P

swiglu_limit = 7.0
swiglu_alpha = 1.702
norm_eps = 1e-05

CHIPS = 32
SIDE = 4
CAP = 12
TOK = 256
ROWS = CHIPS * CAP
SLAB = SIDE * CAP
LANES = 128
BLOCK = SIDE * LANES
BF = jnp.bfloat16
F32 = jnp.float32


def clamped_units(gate_pre, up_pre):
    capped = jnp.minimum(gate_pre, swiglu_limit)
    linear = jnp.clip(up_pre, -swiglu_limit, swiglu_limit)
    return capped * jax.nn.sigmoid(swiglu_alpha * capped) * (linear + 1.0)


def row_labels(shape):
    r = lax.broadcasted_iota(jnp.int32, shape, 0)
    e = (r * 1366) >> 16
    rest = r - e * SLAB
    cb = (rest * 86) >> 10
    return e, cb, rest - cb * CAP


def slot_matches(ids_ref, x):
    shape = (ROWS * SIDE, TOK)
    e, cb, slot = row_labels(shape)
    name = e * SIDE + x
    hits = [name == ids_ref[k : k + 1, :] for k in range(4)]
    named = hits[0] | hits[1] | hits[2] | hits[3]
    before = lax.broadcasted_iota(jnp.int32, (TOK, TOK), 0) < lax.broadcasted_iota(
        jnp.int32, (TOK, TOK), 1
    )
    rank = jnp.dot(
        jnp.where(named, 1.0, 0.0).astype(BF),
        jnp.where(before, 1.0, 0.0).astype(BF),
        preferred_element_type=F32,
    )
    placed = named & (rank == slot.astype(F32))
    return placed, hits, cb


def prep_kernel(pos_ref, tok_ref, gain_ref, ids_ref, out_ref):
    x, y = pos_ref[0], pos_ref[1]
    values = tok_ref[...].astype(F32)
    row_mean = jnp.mean(values, axis=1, keepdims=True)
    centred = values - row_mean
    row_var = jnp.mean(centred * centred, axis=1, keepdims=True)
    cols = pl.ds(pl.multiple_of(y * BLOCK, BLOCK), BLOCK)
    own = tok_ref[:, cols].astype(F32) - row_mean
    normed = (own * lax.rsqrt(row_var + norm_eps) * gain_ref[:, cols]).astype(BF)
    placed, _, cb = slot_matches(ids_ref, x)
    wide = jnp.dot(
        jnp.where(placed, 1.0, 0.0).astype(BF), normed, preferred_element_type=F32
    )
    cb = cb[:, :LANES]
    parts = [wide[:, i * LANES : (i + 1) * LANES] for i in range(SIDE)]
    out = jnp.where(
        cb < 2, jnp.where(cb == 0, parts[0], parts[1]), jnp.where(cb == 2, parts[2], parts[3])
    )
    out_ref[...] = out.astype(BF)


GROUP = 8


def unpack_matrix():
    rows = GROUP * SLAB
    q = np.arange(rows)
    cb, s, slot = q // (GROUP * CAP), q % (GROUP * CAP) // CAP, q % CAP
    m = np.zeros((rows, rows), np.float32)
    m[q, s * SLAB + cb * CAP + slot] = 1.0
    return m


def gate_up_kernel(pos_ref, perm_ref, r0, r1, r2, r3, w0, w1, w2, w3, act_ref, xs):
    y, j = pos_ref[1], pos_ref[2]
    n, m = GROUP * SLAB, GROUP * CAP
    for k, raw in enumerate((r0, r1, r2, r3)):
        yk = lax.rem(y - k + SIDE, SIDE)
        for g in range(CHIPS // GROUP):
            part = jnp.dot(
                perm_ref[...], raw[g * n : (g + 1) * n, :], preferred_element_type=F32
            ).astype(BF)
            for cb in range(SIDE):
                cols = pl.ds(pl.multiple_of(yk * BLOCK + cb * LANES, LANES), LANES)
                xs[g * m : (g + 1) * m, cols] = part[cb * m : (cb + 1) * m, :]
    for k, w in enumerate((w0, w1, w2, w3)):
        both = jnp.concatenate([w[0], w[1]], axis=1)
        pre = jnp.dot(xs[...], both, preferred_element_type=F32)
        block = clamped_units(pre[:, :LANES], pre[:, LANES:]).astype(BF)
        xk = lax.rem(j - k + SIDE, SIDE)
        act_ref[:, pl.ds(pl.multiple_of(xk * LANES, LANES), LANES)] = block


def down_kernel(pos_ref, perm_ref, a0, a1, a2, a3, d0, d1, d2, d3, out_ref, acts, res):
    y, j = pos_ref[1], pos_ref[2]
    n, m = GROUP * SLAB, GROUP * CAP
    for k, a in enumerate((a0, a1, a2, a3)):
        yk = lax.rem(y - k + SIDE, SIDE)
        acts[:, pl.ds(pl.multiple_of(yk * BLOCK, BLOCK), BLOCK)] = a[...]
    for h in range(2):
        d, f = ((d0, d1), (d2, d3))[h]
        both = jnp.concatenate([d[...], f[...]], axis=1)
        out = jnp.dot(acts[...], both, preferred_element_type=F32).astype(BF)
        for i in range(2):
            xk = lax.rem(j - (2 * h + i) + SIDE, SIDE)
            res[:, pl.ds(pl.multiple_of(xk * LANES, LANES), LANES)] = out[
                :, i * LANES : (i + 1) * LANES
            ]
    for g in range(CHIPS // GROUP):
        part = jnp.concatenate(
            [
                res[g * m : (g + 1) * m, cb * LANES : (cb + 1) * LANES]
                for cb in range(SIDE)
            ],
            axis=0,
        )
        out_ref[g * n : (g + 1) * n, :] = jnp.dot(
            perm_ref[...], part, preferred_element_type=F32
        ).astype(BF)


def combine_kernel(pos_ref, ids_ref, weight_ref, ret_ref, out_ref):
    x = pos_ref[0]
    placed, hits, cb = slot_matches(ids_ref, x)
    scale = jnp.zeros(placed.shape, F32)
    for k in range(4):
        scale = jnp.where(hits[k], weight_ref[k : k + 1, :], scale)
    scale = jnp.where(placed, scale, 0.0)
    high = scale.astype(BF)
    low = (scale - high.astype(F32)).astype(BF)
    cb = cb[:, :LANES]
    back = ret_ref[...].astype(F32)
    wide = jnp.concatenate(
        [jnp.where(cb == i, back, 0.0).astype(BF) for i in range(SIDE)], axis=1
    )
    over_rows = (((0,), (0,)), ((), ()))
    total = lax.dot_general(high, wide, over_rows, preferred_element_type=F32)
    total += lax.dot_general(low, wide, over_rows, preferred_element_type=F32)
    for i in range(SIDE):
        out_ref[i] = total[:, i * LANES : (i + 1) * LANES].astype(BF)


def call(kernel, out_shape, n_in, name, flops, nbytes, scratch=()):
    return pl.pallas_call(
        kernel,
        name=name,
        out_shape=out_shape,
        in_specs=[pl.BlockSpec(memory_space=pltpu.SMEM)]
        + [pl.BlockSpec(memory_space=pltpu.VMEM)] * (n_in - 1),
        out_specs=pl.BlockSpec(memory_space=pltpu.VMEM),
        scratch_shapes=list(scratch),
        cost_estimate=pl.CostEstimate(
            flops=flops, bytes_accessed=nbytes, transcendentals=0
        ),
    )


def weight_pairs(k):
    pairs = []
    for z in range(CHIPS):
        for c in range(2):
            for y in range(SIDE):
                for x in range(SIDE):
                    j = (x + k) % SIDE
                    src = (2 * z + c) * 16 + SIDE * y + x
                    dst = (2 * z + j // 2) * 16 + SIDE * y + 2 * c + j % 2
                    pairs.append((src, dst))
    return pairs


def y_pairs(k):
    return [
        (SIDE * y + x, SIDE * ((y + k) % SIDE) + x)
        for y in range(SIDE)
        for x in range(SIDE)
    ]


CORE_GROUPS = [[2 * z + c for z in range(CHIPS)] for c in range(2)]
X_GROUPS = [[SIDE * y + x for x in range(SIDE)] for y in range(SIDE)]


def per_device(tokens, norm_gain, route_ids, route_weights, w_gate, w_up, w_down):
    tp, ep = lax.axis_index("tp"), lax.axis_index("ep")
    x, y, core = tp % SIDE, tp // SIDE, ep % 2
    j = 2 * core + x % 2
    pos = jnp.stack([x, y, j]).astype(jnp.int32)
    mine = x % 2

    def pick(w, i):
        return lax.dynamic_index_in_dim(w, i, 0, keepdims=False)

    gu = [jnp.stack([pick(w_gate, i), pick(w_up, i)]) for i in (mine, 1 - mine)]
    wd = [pick(w_down, i) for i in (mine, 1 - mine)]
    both = ("ep", "tp")
    gu_blocks = [lax.ppermute(gu[k % 2], both, weight_pairs(k)) for k in range(SIDE)]
    wd_blocks = [lax.ppermute(wd[k % 2], both, weight_pairs(k)) for k in range(SIDE)]

    ids_t = route_ids.T
    weights_t = route_weights.T
    slab = jax.ShapeDtypeStruct((ROWS * SIDE, LANES), BF)
    outgoing = call(prep_kernel, slab, 4, "prep", 10**9, 2 * 10**6)(
        pos, tokens, norm_gain.reshape(1, -1), ids_t
    )

    def exchange(a):
        a = a.reshape(CHIPS, SLAB, LANES)
        a = lax.all_to_all(a, "ep", 0, 0, tiled=True, axis_index_groups=CORE_GROUPS)
        return a.reshape(ROWS * SIDE, LANES)

    raw = exchange(outgoing)
    raws = [raw] + [lax.ppermute(raw, "tp", y_pairs(k)) for k in range(1, SIDE)]
    perm = unpack_matrix()
    act = call(
        gate_up_kernel,
        jax.ShapeDtypeStruct((ROWS, BLOCK), BF),
        10,
        "gate_up",
        2 * 10**9,
        6 * 10**6,
        [pltpu.VMEM((ROWS, SIDE * BLOCK), BF)],
    )(pos, jnp.asarray(perm, BF), *raws, *gu_blocks)
    acts = [act] + [lax.ppermute(act, "tp", y_pairs(k)) for k in range(1, SIDE)]
    result = call(
        down_kernel,
        slab,
        10,
        "down",
        10**9,
        4 * 10**6,
        [pltpu.VMEM((ROWS, SIDE * BLOCK), BF), pltpu.VMEM((ROWS, BLOCK), BF)],
    )(pos, jnp.asarray(perm.T, BF), *acts, *wd_blocks)
    returned = exchange(result)
    partial = call(
        combine_kernel,
        jax.ShapeDtypeStruct((SIDE, TOK, LANES), BF),
        4,
        "combine",
        10**9,
        2 * 10**6,
    )(pos, ids_t, weights_t, returned)
    sums = lax.all_to_all(partial, "tp", 0, 0, tiled=True, axis_index_groups=X_GROUPS)
    return jnp.sum(sums.astype(F32), axis=0).astype(BF)


def solution(mesh):
    return jax.shard_map(
        per_device,
        mesh=mesh,
        in_specs=(
            P("ep", None),
            P(),
            P("ep", None),
            P("ep", None),
            P("ep", None, "tp"),
            P("ep", None, "tp"),
            P("ep", None, "tp"),
        ),
        out_specs=P("ep", "tp"),
        check_vma=False,
    )
```

```python
import jax
import jax.numpy as jnp
import numpy as np
from jax import lax
from jax.experimental import pallas as pl
from jax.experimental.pallas import tpu as pltpu
from jax.sharding import PartitionSpec as P

swiglu_limit = 7.0
swiglu_alpha = 1.702
norm_eps = 1e-05

CHIPS = 32
SIDE = 4
PLANE = SIDE * SIDE
CAP = 12
TOK = 256
ROWS = CHIPS * CAP
UNIT = 2 * CAP
SLAB = SIDE * CAP
HALF = 1024
LANES = 128
BLOCK = SIDE * LANES
BF = jnp.bfloat16
F32 = jnp.float32


def clamped_units(gate_pre, up_pre):
    capped = jnp.minimum(gate_pre, swiglu_limit)
    linear = jnp.clip(up_pre, -swiglu_limit, swiglu_limit)
    return capped * jax.nn.sigmoid(swiglu_alpha * capped) * (linear + 1.0)


def iota(shape, dim):
    return lax.broadcasted_iota(jnp.int32, shape, dim)


def as_bf(mask):
    return jnp.where(mask, 1.0, 0.0).astype(BF)


def prep_kernel(pos_ref, tok_ref, gain_ref, ids_ref, out0_ref, out1_ref):
    values = tok_ref[...].astype(F32)
    row_mean = jnp.mean(values, axis=1, keepdims=True)
    centred = values - row_mean
    row_var = jnp.mean(centred * centred, axis=1, keepdims=True)
    normed = (centred * lax.rsqrt(row_var + norm_eps) * gain_ref[...]).astype(BF)
    shape = (2 * SIDE * UNIT, TOK)
    r = iota(shape, 0)
    second = r >= SIDE * UNIT
    rest = jnp.where(second, r - SIDE * UNIT, r)
    q = (rest * 2731) >> 16
    rest = rest - q * UNIT
    half = rest >= CAP
    slot = jnp.where(half, rest - CAP, rest)
    name = jnp.where(second, pos_ref[4], pos_ref[3]) * SIDE + q
    named = name == ids_ref[0:1, :]
    for k in range(1, 4):
        named = named | (name == ids_ref[k : k + 1, :])
    before = as_bf(iota((TOK, TOK), 0) < iota((TOK, TOK), 1))
    rank = jnp.dot(as_bf(named), before, preferred_element_type=F32)
    placed = as_bf(named & (rank == slot.astype(F32)))
    wide = jnp.dot(placed, normed, preferred_element_type=F32)
    upper = half[:, :1]
    out = jnp.where(upper, wide[:, HALF:], wide[:, :HALF]).astype(BF)
    out0_ref[...] = out[: SIDE * UNIT]
    out1_ref[...] = out[SIDE * UNIT :]


def scale_kernel(ids_ref, weight_ref, out_ref):
    shape = (TOK, 4 * ROWS)
    r = iota(shape, 1)
    name = (r * 5462) >> 16
    slot = r - name * CAP
    named = jnp.zeros(shape, jnp.bool_)
    scale = jnp.zeros(shape, F32)
    for k in range(4):
        hit = name == ids_ref[:, k : k + 1]
        named = named | hit
        scale = jnp.where(hit, weight_ref[:, k : k + 1], scale)
    before = as_bf(iota((TOK, TOK), 1) < iota((TOK, TOK), 0))
    rank = jnp.dot(before, as_bf(named), preferred_element_type=F32)
    scale = jnp.where(named & (rank == slot.astype(F32)), scale, 0.0)
    high = scale.astype(BF)
    out_ref[0] = high
    out_ref[1] = (scale - high.astype(F32)).astype(BF)


def combine_kernel(scale_ref, ret_ref, out_ref):
    back = ret_ref[...]
    total = jnp.dot(scale_ref[0], back, preferred_element_type=F32)
    total += jnp.dot(scale_ref[1], back, preferred_element_type=F32)
    out_ref[...] = total.astype(BF)


GROUP = 4


def unpack_matrix():
    n = GROUP * 2 * UNIT
    q = np.arange(n)
    half, unit, slot = q // (n // 2), q % (n // 2) // CAP, q % CAP
    m = np.zeros((n, n), np.float32)
    m[q, unit * UNIT + half * CAP + slot] = 1.0
    return m


def pack_matrix():
    n = GROUP * SLAB
    q = np.arange(n)
    unit, cb, slot = q // SLAB, q % SLAB // CAP, q % CAP
    m = np.zeros((n, n), np.float32)
    m[q, cb * SLAB + unit * CAP + slot] = 1.0
    return m


def gate_up_kernel(pos_ref, perm_ref, raw_ref, w0, w1, v0, v1, act_ref, xs):
    core, x = pos_ref[0], pos_ref[1]
    n = GROUP * 2 * UNIT
    for g in range(PLANE // GROUP):
        part = jnp.dot(
            perm_ref[...], raw_ref[g * n : (g + 1) * n, :], preferred_element_type=F32
        ).astype(BF)
        rows = slice(g * n // 2, (g + 1) * n // 2)
        xs[rows, :HALF] = part[: n // 2]
        xs[rows, HALF:] = part[n // 2 :]
    for k, (own, w) in enumerate(((1, w0), (1, w1), (0, v0), (0, v1))):
        both = jnp.concatenate([w[0], w[1]], axis=1)
        pre = jnp.dot(xs[...], both, preferred_element_type=F32)
        block = clamped_units(pre[:, :LANES], pre[:, LANES:]).astype(BF)
        col = 2 * ((x + k) % 2) + (core if own else 1 - core)
        cols = pl.ds(pl.multiple_of(col * LANES, LANES), LANES)
        for i in range(SIDE):
            act_ref[i, :, cols] = block


def down_kernel(pos_ref, perm_ref, acts, d0, d1, e0, e1, out_ref, res):
    core, x, z = pos_ref[0], pos_ref[1], pos_ref[2]
    for own, pair in ((1, (d0, d1)), (0, (e0, e1))):
        total = jnp.zeros((ROWS, 2 * LANES), F32)
        for i in range(SIDE):
            rows = slice(i * BLOCK, (i + 1) * BLOCK)
            both = jnp.concatenate([pair[0][rows, :], pair[1][rows, :]], axis=1)
            total += jnp.dot(acts[i], both, preferred_element_type=F32)
        out = total.astype(BF)
        for k in range(2):
            col = 2 * ((x + k) % 2) + (core if own else 1 - core)
            cols = pl.ds(pl.multiple_of(col * LANES, LANES), LANES)
            res[:, cols] = out[:, k * LANES : (k + 1) * LANES]
    sign = 1 - 2 * core
    for g in range(CHIPS // GROUP):
        rows = slice(g * SLAB, (g + 1) * SLAB)
        part = jnp.concatenate(
            [res[rows, cb * LANES : (cb + 1) * LANES] for cb in range(SIDE)], axis=0
        )
        part = jnp.dot(perm_ref[...], part, preferred_element_type=F32).astype(BF)
        for i in range(GROUP):
            t, m = divmod(g * GROUP + i, 2)
            shift = sign * (-(15 - t) if m else t + 1)
            source = (z - shift + 2 * CHIPS) % CHIPS
            out_ref[pl.ds(pl.multiple_of(source * SLAB, SLAB), SLAB), :] = part[
                i * SLAB : (i + 1) * SLAB
            ]


def call(kernel, out_shape, n_in, flops, nbytes, scratch=(), scalars=True):
    vmem = pl.BlockSpec(memory_space=pltpu.VMEM)
    first = [pl.BlockSpec(memory_space=pltpu.SMEM)] if scalars else []
    return pl.pallas_call(
        kernel,
        out_shape=out_shape,
        in_specs=first + [vmem] * (n_in - len(first)),
        out_specs=jax.tree.map(lambda _: vmem, out_shape),
        scratch_shapes=list(scratch),
        compiler_params=pltpu.CompilerParams(vmem_limit_bytes=24 * 2**20),
        cost_estimate=pl.CostEstimate(
            flops=flops, bytes_accessed=nbytes, transcendentals=0
        ),
    )


def devices():
    for z in range(CHIPS):
        for c in range(2):
            for y in range(SIDE):
                for x in range(SIDE):
                    yield z, c, y, x


def at(z, c, y, x):
    return (2 * (z % CHIPS) + c) * PLANE + SIDE * y + x


def shift_of(m, c, t):
    s = -(15 - t) if m else t + 1
    return s if c == 0 else -s


def z_pairs(m):
    return [
        (at(z, c, y, x), at(z + shift_of(m, c, SIDE * y + x), c, y, x))
        for z, c, y, x in devices()
    ]


def weight_pairs(k):
    return [
        (at(z, c, y, x), at(z, x % 2, y, 2 * c + (x // 2 + k) % 2))
        for z, c, y, x in devices()
    ]


SIBLING = [(at(z, c, y, x), at(z, 1 - c, y, x)) for z, c, y, x in devices()]
Y_GROUPS = [[SIDE * y + x for y in range(SIDE)] for x in range(SIDE)]
BACK_GROUPS = [
    [at(z, c, y, x) for z in range(CHIPS) for x in range(SIDE)]
    for c in range(2)
    for y in range(SIDE)
]
BOTH = ("ep", "tp")


def permute(a, pairs):
    return lax.ppermute(a, BOTH, pairs)


def per_device(tokens, norm_gain, route_ids, route_weights, w_gate, w_up, w_down):
    tp, ep = lax.axis_index("tp"), lax.axis_index("ep")
    x, z, core = tp & 3, ep >> 1, ep & 1
    sign = 1 - 2 * core
    pos = jnp.stack(
        [core, x, z, (z + sign * (tp + 1)) & 31, (z - sign * (15 - tp)) & 31]
    ).astype(jnp.int32)

    message = jax.ShapeDtypeStruct((SIDE * UNIT, HALF), BF)
    out0, out1 = call(prep_kernel, (message, message), 4, 10**8, 2 * 10**6)(
        pos, tokens, norm_gain.reshape(1, -1), route_ids.T
    )
    got = [permute(out, z_pairs(m)) for m, out in enumerate((out0, out1))]

    def pick(w, i):
        return lax.dynamic_index_in_dim(w, i, 0, keepdims=False)

    def share(blocks):
        own = [permute(blocks[k], weight_pairs(k)) for k in range(2)]
        return own + [permute(b, SIBLING) for b in own]

    mine = (tp >> 1) & 1
    gu_blocks = share(
        [jnp.stack([pick(w_gate, i), pick(w_up, i)]) for i in (mine, 1 - mine)]
    )
    wd_blocks = share([pick(w_down, i) for i in (mine, 1 - mine)])
    scale = call(
        scale_kernel,
        jax.ShapeDtypeStruct((2, TOK, 4 * ROWS), BF),
        2,
        10**8,
        2 * 10**6,
        scalars=False,
    )(route_ids, route_weights)

    units = jnp.concatenate([g.reshape(SIDE, UNIT, HALF) for g in got], axis=1)
    units = jnp.broadcast_to(units[None], (SIDE, SIDE, 2 * UNIT, HALF))
    raw = lax.all_to_all(
        units.reshape(PLANE, 2 * UNIT, HALF), "tp", 0, 0, tiled=True
    ).reshape(2 * ROWS, HALF)
    act = call(
        gate_up_kernel,
        jax.ShapeDtypeStruct((SIDE, ROWS, BLOCK), BF),
        7,
        2 * 10**9,
        6 * 10**6,
        [pltpu.VMEM((ROWS, 2 * HALF), BF)],
    )(pos, jnp.asarray(unpack_matrix(), BF), raw, *gu_blocks)
    acts = lax.all_to_all(act, "tp", 0, 0, tiled=True, axis_index_groups=Y_GROUPS)
    result = call(
        down_kernel,
        jax.ShapeDtypeStruct((4 * ROWS, LANES), BF),
        7,
        10**9,
        4 * 10**6,
        [pltpu.VMEM((ROWS, BLOCK), BF)],
    )(pos, jnp.asarray(pack_matrix(), BF), acts, *wd_blocks)
    returned = lax.all_to_all(
        result.reshape(4 * CHIPS, 3, 4, LANES),
        BOTH,
        0,
        0,
        tiled=True,
        axis_index_groups=BACK_GROUPS,
    ).reshape(4 * ROWS, LANES)
    return call(
        combine_kernel,
        jax.ShapeDtypeStruct((TOK, LANES), BF),
        2,
        2 * 10**8,
        2 * 10**6,
        scalars=False,
    )(scale, returned)


def solution(mesh):
    return jax.shard_map(
        per_device,
        mesh=mesh,
        in_specs=(
            P("ep", None),
            P(),
            P("ep", None),
            P("ep", None),
            P("ep", None, "tp"),
            P("ep", None, "tp"),
            P("ep", None, "tp"),
        ),
        out_specs=P("ep", "tp"),
        check_vma=False,
    )
```

```python
import jax
import jax.numpy as jnp
import numpy as np
from jax import lax
from jax.experimental import pallas as pl
from jax.experimental.pallas import tpu as pltpu
from jax.sharding import PartitionSpec as P

swiglu_limit = 7.0
swiglu_alpha = 1.702
norm_eps = 1e-05

CHIPS = 32
SIDE = 4
PLANE = SIDE * SIDE
CAP = 12
TOK = 256
ROWS = CHIPS * CAP
UNIT = 2 * CAP
SLAB = SIDE * CAP
HALF = 256
LANES = 128
BLOCK = SIDE * LANES
BF = jnp.bfloat16
F32 = jnp.float32


def clamped_units(gate_pre, up_pre):
    capped = jnp.minimum(gate_pre, swiglu_limit)
    linear = jnp.clip(up_pre, -swiglu_limit, swiglu_limit)
    return capped * jax.nn.sigmoid(swiglu_alpha * capped) * (linear + 1.0)


def iota(shape, dim):
    return lax.broadcasted_iota(jnp.int32, shape, dim)


def as_bf(mask):
    return jnp.where(mask, 1.0, 0.0).astype(BF)


def prep_kernel(pos_ref, tok_ref, gain_ref, ids_ref, out_ref):
    x, y = pos_ref[1], pos_ref[3]
    values = tok_ref[...].astype(F32)
    row_mean = jnp.mean(values, axis=1, keepdims=True)
    centred = values - row_mean
    row_var = jnp.mean(centred * centred, axis=1, keepdims=True)
    cols = pl.ds(pl.multiple_of(y * BLOCK, BLOCK), BLOCK)
    own = tok_ref[:, cols].astype(F32) - row_mean
    normed = (own * lax.rsqrt(row_var + norm_eps) * gain_ref[:, cols]).astype(BF)
    shape = (CHIPS * UNIT, TOK)
    r = iota(shape, 0)
    chip = (r * 2731) >> 16
    rest = r - chip * UNIT
    half = rest >= CAP
    slot = jnp.where(half, rest - CAP, rest)
    name = chip * SIDE + x
    named = name == ids_ref[0:1, :]
    for k in range(1, 4):
        named = named | (name == ids_ref[k : k + 1, :])
    before = as_bf(iota((TOK, TOK), 0) < iota((TOK, TOK), 1))
    rank = jnp.dot(as_bf(named), before, preferred_element_type=F32)
    placed = as_bf(named & (rank == slot.astype(F32)))
    wide = jnp.dot(placed, normed, preferred_element_type=F32)
    out_ref[...] = jnp.where(half[:, :1], wide[:, HALF:], wide[:, :HALF]).astype(BF)


def scale_kernel(ids_ref, weight_ref, out_ref):
    shape = (TOK, 4 * ROWS)
    r = iota(shape, 1)
    name = (r * 5462) >> 16
    slot = r - name * CAP
    named = jnp.zeros(shape, jnp.bool_)
    scale = jnp.zeros(shape, F32)
    for k in range(4):
        hit = name == ids_ref[:, k : k + 1]
        named = named | hit
        scale = jnp.where(hit, weight_ref[:, k : k + 1], scale)
    before = as_bf(iota((TOK, TOK), 1) < iota((TOK, TOK), 0))
    rank = jnp.dot(before, as_bf(named), preferred_element_type=F32)
    scale = jnp.where(named & (rank == slot.astype(F32)), scale, 0.0)
    high = scale.astype(BF)
    out_ref[0] = high
    out_ref[1] = (scale - high.astype(F32)).astype(BF)


def combine_kernel(scale_ref, ret_ref, out_ref):
    back = ret_ref[...]
    total = jnp.dot(scale_ref[0], back, preferred_element_type=F32)
    total += jnp.dot(scale_ref[1], back, preferred_element_type=F32)
    out_ref[...] = total.astype(BF)


GROUP = 4


def unpack_matrix():
    n = 2 * GROUP * UNIT
    q = np.arange(n)
    half, unit, slot = q // (n // 2), q % (n // 2) // CAP, q % CAP
    m = np.zeros((n, n), np.float32)
    m[q, unit * UNIT + half * CAP + slot] = 1.0
    return m


def pack_matrix():
    n = GROUP * SLAB
    q = np.arange(n)
    unit, cb, slot = q // SLAB, q % SLAB // CAP, q % CAP
    m = np.zeros((n, n), np.float32)
    m[q, cb * SLAB + unit * CAP + slot] = 1.0
    return m


def gate_up_kernel(pos_ref, perm_ref, raw_ref, w0, w1, v0, v1, act_ref, xs):
    core, x = pos_ref[0], pos_ref[1]
    n, m = 2 * GROUP * UNIT, 2 * GROUP * CAP
    for y in range(SIDE):
        for g in range(CHIPS // (2 * GROUP)):
            part = jnp.dot(
                perm_ref[...],
                raw_ref[y, g * n : (g + 1) * n, :],
                preferred_element_type=F32,
            ).astype(BF)
            for h in range(2):
                cols = slice((2 * y + h) * HALF, (2 * y + h + 1) * HALF)
                xs[g * m : (g + 1) * m, cols] = part[h * m : (h + 1) * m]
    for k, (own, w) in enumerate(((1, w0), (1, w1), (0, v0), (0, v1))):
        both = jnp.concatenate([w[0], w[1]], axis=1)
        pre = jnp.dot(xs[...], both, preferred_element_type=F32)
        block = clamped_units(pre[:, :LANES], pre[:, LANES:]).astype(BF)
        col = 2 * ((x + k) % 2) + (core if own else 1 - core)
        cols = pl.ds(pl.multiple_of(col * LANES, LANES), LANES)
        for i in range(SIDE):
            act_ref[i, :, cols] = block


def down_kernel(pos_ref, perm_ref, acts, d0, d1, e0, e1, out_ref, res):
    core, x = pos_ref[0], pos_ref[1]
    for own, pair in ((1, (d0, d1)), (0, (e0, e1))):
        total = jnp.zeros((ROWS, 2 * LANES), F32)
        for i in range(SIDE):
            rows = slice(i * BLOCK, (i + 1) * BLOCK)
            both = jnp.concatenate([pair[0][rows, :], pair[1][rows, :]], axis=1)
            total += jnp.dot(acts[i], both, preferred_element_type=F32)
        out = total.astype(BF)
        for k in range(2):
            col = 2 * ((x + k) % 2) + (core if own else 1 - core)
            cols = pl.ds(pl.multiple_of(col * LANES, LANES), LANES)
            res[:, cols] = out[:, k * LANES : (k + 1) * LANES]
    for g in range(CHIPS // GROUP):
        rows = slice(g * SLAB, (g + 1) * SLAB)
        part = jnp.concatenate(
            [res[rows, cb * LANES : (cb + 1) * LANES] for cb in range(SIDE)], axis=0
        )
        n = GROUP * SLAB
        out_ref[g * n : (g + 1) * n, :] = jnp.dot(
            perm_ref[...], part, preferred_element_type=F32
        ).astype(BF)


def call(kernel, out_shape, n_in, flops, nbytes, scratch=(), scalars=True):
    vmem = pl.BlockSpec(memory_space=pltpu.VMEM)
    first = [pl.BlockSpec(memory_space=pltpu.SMEM)] if scalars else []
    return pl.pallas_call(
        kernel,
        out_shape=out_shape,
        in_specs=first + [vmem] * (n_in - len(first)),
        out_specs=jax.tree.map(lambda _: vmem, out_shape),
        scratch_shapes=list(scratch),
        compiler_params=pltpu.CompilerParams(vmem_limit_bytes=24 * 2**20),
        cost_estimate=pl.CostEstimate(
            flops=flops, bytes_accessed=nbytes, transcendentals=0
        ),
    )


def devices():
    for z in range(CHIPS):
        for c in range(2):
            for y in range(SIDE):
                for x in range(SIDE):
                    yield z, c, y, x


def at(z, c, y, x):
    return (2 * (z % CHIPS) + c) * PLANE + SIDE * y + x


def weight_pairs(k):
    return [
        (at(z, c, y, x), at(z, x % 2, y, 2 * c + (x // 2 + k) % 2))
        for z, c, y, x in devices()
    ]


SIBLING = [(at(z, c, y, x), at(z, 1 - c, y, x)) for z, c, y, x in devices()]
CORE_GROUPS = [[2 * z + c for z in range(CHIPS)] for c in range(2)]
Y_GROUPS = [[SIDE * y + x for y in range(SIDE)] for x in range(SIDE)]
BACK_GROUPS = [
    [at(z, c, y, x) for z in range(CHIPS) for x in range(SIDE)]
    for c in range(2)
    for y in range(SIDE)
]
BOTH = ("ep", "tp")


def permute(a, pairs):
    return lax.ppermute(a, BOTH, pairs)


def exchange(a, axes, groups):
    return lax.all_to_all(a, axes, 0, 0, tiled=True, axis_index_groups=groups)


def per_device(tokens, norm_gain, route_ids, route_weights, w_gate, w_up, w_down):
    tp, ep = lax.axis_index("tp"), lax.axis_index("ep")
    x, z, core = tp & 3, ep >> 1, ep & 1
    pos = jnp.stack([core, x, z, tp >> 2]).astype(jnp.int32)
    outgoing = call(
        prep_kernel, jax.ShapeDtypeStruct((CHIPS * UNIT, HALF), BF), 4, 10**8, 2 * 10**6
    )(pos, tokens, norm_gain.reshape(1, -1), route_ids.T)
    raw = exchange(outgoing.reshape(CHIPS, UNIT, HALF), "ep", CORE_GROUPS)

    def pick(w, i):
        return lax.dynamic_index_in_dim(w, i, 0, keepdims=False)

    def share(blocks):
        own = [permute(blocks[k], weight_pairs(k)) for k in range(2)]
        return own + [permute(b, SIBLING) for b in own]

    mine = (tp >> 1) & 1
    gu_blocks = share(
        [jnp.stack([pick(w_gate, i), pick(w_up, i)]) for i in (mine, 1 - mine)]
    )
    wd_blocks = share([pick(w_down, i) for i in (mine, 1 - mine)])
    scale = call(
        scale_kernel,
        jax.ShapeDtypeStruct((2, TOK, 4 * ROWS), BF),
        2,
        10**8,
        2 * 10**6,
        scalars=False,
    )(route_ids, route_weights)

    raw = jnp.broadcast_to(
        raw.reshape(1, CHIPS * UNIT, HALF), (SIDE, CHIPS * UNIT, HALF)
    )
    raw = exchange(raw, "tp", Y_GROUPS)
    act = call(
        gate_up_kernel,
        jax.ShapeDtypeStruct((SIDE, ROWS, BLOCK), BF),
        7,
        2 * 10**9,
        6 * 10**6,
        [pltpu.VMEM((ROWS, SIDE * BLOCK), BF)],
    )(pos, jnp.asarray(unpack_matrix(), BF), raw, *gu_blocks)
    acts = exchange(act, "tp", Y_GROUPS)
    result = call(
        down_kernel,
        jax.ShapeDtypeStruct((4 * ROWS, LANES), BF),
        7,
        10**9,
        4 * 10**6,
        [pltpu.VMEM((ROWS, BLOCK), BF)],
    )(pos, jnp.asarray(pack_matrix(), BF), acts, *wd_blocks)
    returned = exchange(
        result.reshape(4 * CHIPS, 3, 4, LANES), BOTH, BACK_GROUPS
    ).reshape(4 * ROWS, LANES)
    return call(
        combine_kernel,
        jax.ShapeDtypeStruct((TOK, LANES), BF),
        2,
        2 * 10**8,
        2 * 10**6,
        scalars=False,
    )(scale, returned)


def solution(mesh):
    return jax.shard_map(
        per_device,
        mesh=mesh,
        in_specs=(
            P("ep", None),
            P(),
            P("ep", None),
            P("ep", None),
            P("ep", None, "tp"),
            P("ep", None, "tp"),
            P("ep", None, "tp"),
        ),
        out_specs=P("ep", "tp"),
        check_vma=False,
    )
```

```python
import jax
import jax.numpy as jnp
import numpy as np
from jax import lax
from jax.experimental import pallas as pl
from jax.experimental.pallas import tpu as pltpu
from jax.sharding import PartitionSpec as P

swiglu_limit = 7.0
swiglu_alpha = 1.702
norm_eps = 1e-05

CHIPS = 32
SIDE = 4
PLANE = SIDE * SIDE
CAP = 12
FIRST = 16
STEP = 1
TOK = 256
ROWS = CHIPS * CAP
UNIT = 2 * CAP
SLAB = SIDE * CAP
HALF = 256
LANES = 128
BLOCK = SIDE * LANES
BF = jnp.bfloat16
F32 = jnp.float32


def clamped_units(gate_pre, up_pre):
    capped = jnp.minimum(gate_pre, swiglu_limit)
    linear = jnp.clip(up_pre, -swiglu_limit, swiglu_limit)
    return capped * jax.nn.sigmoid(swiglu_alpha * capped) * (linear + 1.0)


def iota(shape, dim):
    return lax.broadcasted_iota(jnp.int32, shape, dim)


def as_bf(mask):
    return jnp.where(mask, 1.0, 0.0).astype(BF)


def prep_kernel(pos_ref, tok_ref, gain_ref, ids_ref, out_ref):
    x, y = pos_ref[1], pos_ref[3]
    values = tok_ref[...].astype(F32)
    row_mean = jnp.mean(values, axis=1, keepdims=True)
    centred = values - row_mean
    row_var = jnp.mean(centred * centred, axis=1, keepdims=True)
    cols = pl.ds(pl.multiple_of(y * BLOCK, BLOCK), BLOCK)
    own = tok_ref[:, cols].astype(F32) - row_mean
    normed = (own * lax.rsqrt(row_var + norm_eps) * gain_ref[:, cols]).astype(BF)
    shape = (CHIPS * UNIT, TOK)
    r = iota(shape, 0)
    chip = (r * 2731) >> 16
    rest = r - chip * UNIT
    half = rest >= CAP
    slot = jnp.where(half, rest - CAP, rest)
    name = ((chip * STEP + FIRST) & (CHIPS - 1)) * SIDE + x
    named = name == ids_ref[0:1, :]
    for k in range(1, 4):
        named = named | (name == ids_ref[k : k + 1, :])
    before = as_bf(iota((TOK, TOK), 0) < iota((TOK, TOK), 1))
    rank = jnp.dot(as_bf(named), before, preferred_element_type=F32)
    placed = as_bf(named & (rank == slot.astype(F32)))
    wide = jnp.dot(placed, normed, preferred_element_type=F32)
    out_ref[...] = jnp.where(half[:, :1], wide[:, HALF:], wide[:, :HALF]).astype(BF)


def scale_kernel(ids_ref, weight_ref, out_ref):
    shape = (TOK, 4 * ROWS)
    r = iota(shape, 1)
    name = (r * 5462) >> 16
    slot = r - name * CAP
    chip = ((name >> 2) * STEP + FIRST) & (CHIPS - 1)
    name = chip * SIDE + (name & (SIDE - 1))
    named = jnp.zeros(shape, jnp.bool_)
    scale = jnp.zeros(shape, F32)
    for k in range(4):
        hit = name == ids_ref[:, k : k + 1]
        named = named | hit
        scale = jnp.where(hit, weight_ref[:, k : k + 1], scale)
    before = as_bf(iota((TOK, TOK), 1) < iota((TOK, TOK), 0))
    rank = jnp.dot(before, as_bf(named), preferred_element_type=F32)
    scale = jnp.where(named & (rank == slot.astype(F32)), scale, 0.0)
    high = scale.astype(BF)
    out_ref[0] = high
    out_ref[1] = (scale - high.astype(F32)).astype(BF)


def combine_kernel(scale_ref, ret_ref, out_ref):
    back = ret_ref[...]
    total = jnp.dot(scale_ref[0], back, preferred_element_type=F32)
    total += jnp.dot(scale_ref[1], back, preferred_element_type=F32)
    out_ref[...] = total.astype(BF)


GROUP = 4


def unpack_matrix():
    n = 2 * GROUP * UNIT
    q = np.arange(n)
    half, unit, slot = q // (n // 2), q % (n // 2) // CAP, q % CAP
    m = np.zeros((n, n), np.float32)
    m[q, unit * UNIT + half * CAP + slot] = 1.0
    return m


def pack_matrix():
    n = GROUP * SLAB
    q = np.arange(n)
    unit, cb, slot = q // SLAB, q % SLAB // CAP, q % CAP
    m = np.zeros((n, n), np.float32)
    m[q, cb * SLAB + unit * CAP + slot] = 1.0
    return m


def gate_up_kernel(pos_ref, perm_ref, raw_ref, w0, w1, v0, v1, act_ref, xs):
    core, x = pos_ref[0], pos_ref[1]
    n, m = 2 * GROUP * UNIT, 2 * GROUP * CAP
    for y in range(SIDE):
        for g in range(CHIPS // (2 * GROUP)):
            part = jnp.dot(
                perm_ref[...],
                raw_ref[y, g * n : (g + 1) * n, :],
                preferred_element_type=F32,
            ).astype(BF)
            for h in range(2):
                cols = slice((2 * y + h) * HALF, (2 * y + h + 1) * HALF)
                xs[g * m : (g + 1) * m, cols] = part[h * m : (h + 1) * m]
    for k, (own, w) in enumerate(((1, w0), (1, w1), (0, v0), (0, v1))):
        both = jnp.concatenate([w[0], w[1]], axis=1)
        pre = jnp.dot(xs[...], both, preferred_element_type=F32)
        block = clamped_units(pre[:, :LANES], pre[:, LANES:]).astype(BF)
        col = 2 * ((x + k) % 2) + (core if own else 1 - core)
        cols = pl.ds(pl.multiple_of(col * LANES, LANES), LANES)
        for i in range(SIDE):
            act_ref[i, :, cols] = block


def down_kernel(pos_ref, perm_ref, acts, d0, d1, e0, e1, out_ref, res):
    core, x = pos_ref[0], pos_ref[1]
    for own, pair in ((1, (d0, d1)), (0, (e0, e1))):
        total = jnp.zeros((ROWS, 2 * LANES), F32)
        for i in range(SIDE):
            rows = slice(i * BLOCK, (i + 1) * BLOCK)
            both = jnp.concatenate([pair[0][rows, :], pair[1][rows, :]], axis=1)
            total += jnp.dot(acts[i], both, preferred_element_type=F32)
        out = total.astype(BF)
        for k in range(2):
            col = 2 * ((x + k) % 2) + (core if own else 1 - core)
            cols = pl.ds(pl.multiple_of(col * LANES, LANES), LANES)
            res[:, cols] = out[:, k * LANES : (k + 1) * LANES]
    for g in range(CHIPS // GROUP):
        rows = slice(g * SLAB, (g + 1) * SLAB)
        part = jnp.concatenate(
            [res[rows, cb * LANES : (cb + 1) * LANES] for cb in range(SIDE)], axis=0
        )
        n = GROUP * SLAB
        out_ref[g * n : (g + 1) * n, :] = jnp.dot(
            perm_ref[...], part, preferred_element_type=F32
        ).astype(BF)


def call(kernel, out_shape, n_in, flops, nbytes, scratch=(), scalars=True):
    vmem = pl.BlockSpec(memory_space=pltpu.VMEM)
    first = [pl.BlockSpec(memory_space=pltpu.SMEM)] if scalars else []
    return pl.pallas_call(
        kernel,
        out_shape=out_shape,
        in_specs=first + [vmem] * (n_in - len(first)),
        out_specs=jax.tree.map(lambda _: vmem, out_shape),
        scratch_shapes=list(scratch),
        compiler_params=pltpu.CompilerParams(vmem_limit_bytes=24 * 2**20),
        cost_estimate=pl.CostEstimate(
            flops=flops, bytes_accessed=nbytes, transcendentals=0
        ),
    )


def devices():
    for z in range(CHIPS):
        for c in range(2):
            for y in range(SIDE):
                for x in range(SIDE):
                    yield z, c, y, x


def at(z, c, y, x):
    return (2 * (z % CHIPS) + c) * PLANE + SIDE * y + x


def weight_pairs(k):
    return [
        (at(z, c, y, x), at(z, x % 2, y, 2 * c + (x // 2 + k) % 2))
        for z, c, y, x in devices()
    ]


SIBLING = [(at(z, c, y, x), at(z, 1 - c, y, x)) for z, c, y, x in devices()]
ORDER = [(i * STEP + FIRST) % CHIPS for i in range(CHIPS)]
CORE_GROUPS = [[2 * z + c for z in ORDER] for c in range(2)]
Y_GROUPS = [[SIDE * y + x for y in range(SIDE)] for x in range(SIDE)]
BACK_GROUPS = [
    [at(z, c, y, x) for z in ORDER for x in range(SIDE)]
    for c in range(2)
    for y in range(SIDE)
]
BOTH = ("ep", "tp")


def permute(a, pairs):
    return lax.ppermute(a, BOTH, pairs)


def exchange(a, axes, groups):
    return lax.all_to_all(a, axes, 0, 0, tiled=True, axis_index_groups=groups)


def per_device(tokens, norm_gain, route_ids, route_weights, w_gate, w_up, w_down):
    tp, ep = lax.axis_index("tp"), lax.axis_index("ep")
    x, z, core = tp & 3, ep >> 1, ep & 1
    pos = jnp.stack([core, x, z, tp >> 2]).astype(jnp.int32)
    outgoing = call(
        prep_kernel, jax.ShapeDtypeStruct((CHIPS * UNIT, HALF), BF), 4, 10**8, 2 * 10**6
    )(pos, tokens, norm_gain.reshape(1, -1), route_ids.T)
    raw = exchange(outgoing.reshape(CHIPS, UNIT, HALF), "ep", CORE_GROUPS)

    def pick(w, i):
        return lax.dynamic_index_in_dim(w, i, 0, keepdims=False)

    def share(blocks):
        own = [permute(blocks[k], weight_pairs(k)) for k in range(2)]
        return own + [permute(b, SIBLING) for b in own]

    mine = (tp >> 1) & 1
    gu_blocks = share(
        [jnp.stack([pick(w_gate, i), pick(w_up, i)]) for i in (mine, 1 - mine)]
    )
    wd_blocks = share([pick(w_down, i) for i in (mine, 1 - mine)])
    scale = call(
        scale_kernel,
        jax.ShapeDtypeStruct((2, TOK, 4 * ROWS), BF),
        2,
        10**8,
        2 * 10**6,
        scalars=False,
    )(route_ids, route_weights)

    raw = jnp.broadcast_to(
        raw.reshape(1, CHIPS * UNIT, HALF), (SIDE, CHIPS * UNIT, HALF)
    )
    raw = exchange(raw, "tp", Y_GROUPS)
    act = call(
        gate_up_kernel,
        jax.ShapeDtypeStruct((SIDE, ROWS, BLOCK), BF),
        7,
        2 * 10**9,
        6 * 10**6,
        [pltpu.VMEM((ROWS, SIDE * BLOCK), BF)],
    )(pos, jnp.asarray(unpack_matrix(), BF), raw, *gu_blocks)
    acts = exchange(act, "tp", Y_GROUPS)
    result = call(
        down_kernel,
        jax.ShapeDtypeStruct((4 * ROWS, LANES), BF),
        7,
        10**9,
        4 * 10**6,
        [pltpu.VMEM((ROWS, BLOCK), BF)],
    )(pos, jnp.asarray(pack_matrix(), BF), acts, *wd_blocks)
    returned = exchange(
        result.reshape(4 * CHIPS, 3, 4, LANES), BOTH, BACK_GROUPS
    ).reshape(4 * ROWS, LANES)
    return call(
        combine_kernel,
        jax.ShapeDtypeStruct((TOK, LANES), BF),
        2,
        2 * 10**8,
        2 * 10**6,
        scalars=False,
    )(scale, returned)


def solution(mesh):
    return jax.shard_map(
        per_device,
        mesh=mesh,
        in_specs=(
            P("ep", None),
            P(),
            P("ep", None),
            P("ep", None),
            P("ep", None, "tp"),
            P("ep", None, "tp"),
            P("ep", None, "tp"),
        ),
        out_specs=P("ep", "tp"),
        check_vma=False,
    )
```

```python
import jax
import jax.numpy as jnp
import numpy as np
from jax import lax
from jax.experimental import pallas as pl
from jax.experimental.pallas import tpu as pltpu
from jax.sharding import PartitionSpec as P

swiglu_limit = 7.0
swiglu_alpha = 1.702
norm_eps = 1e-05

CHIPS = 32
SIDE = 4
PLANE = SIDE * SIDE
CAP = 12
FIRST = 20
STEP = 1
TOK = 256
ROWS = CHIPS * CAP
UNIT = 2 * CAP
SLAB = SIDE * CAP
HALF = 256
LANES = 128
BLOCK = SIDE * LANES
BF = jnp.bfloat16
F32 = jnp.float32


def clamped_units(gate_pre, up_pre):
    capped = jnp.minimum(gate_pre, swiglu_limit)
    linear = jnp.clip(up_pre, -swiglu_limit, swiglu_limit)
    return capped * jax.nn.sigmoid(swiglu_alpha * capped) * (linear + 1.0)


def iota(shape, dim):
    return lax.broadcasted_iota(jnp.int32, shape, dim)


def as_bf(mask):
    return jnp.where(mask, 1.0, 0.0).astype(BF)


def prep_kernel(pos_ref, tok_ref, gain_ref, ids_ref, out_ref):
    x, y = pos_ref[1], pos_ref[3]
    values = tok_ref[...].astype(F32)
    row_mean = jnp.mean(values, axis=1, keepdims=True)
    centred = values - row_mean
    row_var = jnp.mean(centred * centred, axis=1, keepdims=True)
    cols = pl.ds(pl.multiple_of(y * BLOCK, BLOCK), BLOCK)
    own = tok_ref[:, cols].astype(F32) - row_mean
    normed = (own * lax.rsqrt(row_var + norm_eps) * gain_ref[:, cols]).astype(BF)
    shape = (CHIPS * UNIT, TOK)
    r = iota(shape, 0)
    chip = (r * 2731) >> 16
    rest = r - chip * UNIT
    half = rest >= CAP
    slot = jnp.where(half, rest - CAP, rest)
    name = ((chip * STEP + FIRST) & (CHIPS - 1)) * SIDE + x
    named = name == ids_ref[0:1, :]
    for k in range(1, 4):
        named = named | (name == ids_ref[k : k + 1, :])
    before = as_bf(iota((TOK, TOK), 0) < iota((TOK, TOK), 1))
    rank = jnp.dot(as_bf(named), before, preferred_element_type=F32)
    placed = as_bf(named & (rank == slot.astype(F32)))
    wide = jnp.dot(placed, normed, preferred_element_type=F32)
    out_ref[...] = jnp.where(half[:, :1], wide[:, HALF:], wide[:, :HALF]).astype(BF)


def scale_kernel(ids_ref, weight_ref, out_ref):
    shape = (TOK, 4 * ROWS)
    r = iota(shape, 1)
    name = (r * 5462) >> 16
    slot = r - name * CAP
    chip = ((name >> 2) * STEP + FIRST) & (CHIPS - 1)
    name = chip * SIDE + (name & (SIDE - 1))
    named = jnp.zeros(shape, jnp.bool_)
    scale = jnp.zeros(shape, F32)
    for k in range(4):
        hit = name == ids_ref[:, k : k + 1]
        named = named | hit
        scale = jnp.where(hit, weight_ref[:, k : k + 1], scale)
    before = as_bf(iota((TOK, TOK), 1) < iota((TOK, TOK), 0))
    rank = jnp.dot(before, as_bf(named), preferred_element_type=F32)
    scale = jnp.where(named & (rank == slot.astype(F32)), scale, 0.0)
    high = scale.astype(BF)
    out_ref[0] = high
    out_ref[1] = (scale - high.astype(F32)).astype(BF)


def combine_kernel(scale_ref, ret_ref, out_ref):
    back = ret_ref[...]
    total = jnp.dot(scale_ref[0], back, preferred_element_type=F32)
    total += jnp.dot(scale_ref[1], back, preferred_element_type=F32)
    out_ref[...] = total.astype(BF)


GROUP = 4


def unpack_matrix():
    n = 2 * GROUP * UNIT
    q = np.arange(n)
    half, unit, slot = q // (n // 2), q % (n // 2) // CAP, q % CAP
    m = np.zeros((n, n), np.float32)
    m[q, unit * UNIT + half * CAP + slot] = 1.0
    return m


def pack_matrix():
    n = GROUP * SLAB
    q = np.arange(n)
    unit, cb, slot = q // SLAB, q % SLAB // CAP, q % CAP
    m = np.zeros((n, n), np.float32)
    m[q, cb * SLAB + unit * CAP + slot] = 1.0
    return m


def gate_up_kernel(pos_ref, perm_ref, raw_ref, w0, w1, v0, v1, act_ref, xs):
    core, x = pos_ref[0], pos_ref[1]
    n, m = 2 * GROUP * UNIT, 2 * GROUP * CAP
    for y in range(SIDE):
        for g in range(CHIPS // (2 * GROUP)):
            part = jnp.dot(
                perm_ref[...],
                raw_ref[y, g * n : (g + 1) * n, :],
                preferred_element_type=F32,
            ).astype(BF)
            for h in range(2):
                cols = slice((2 * y + h) * HALF, (2 * y + h + 1) * HALF)
                xs[g * m : (g + 1) * m, cols] = part[h * m : (h + 1) * m]
    for k, (own, w) in enumerate(((1, w0), (1, w1), (0, v0), (0, v1))):
        both = jnp.concatenate([w[0], w[1]], axis=1)
        pre = jnp.dot(xs[...], both, preferred_element_type=F32)
        block = clamped_units(pre[:, :LANES], pre[:, LANES:]).astype(BF)
        col = 2 * ((x + k) % 2) + (core if own else 1 - core)
        cols = pl.ds(pl.multiple_of(col * LANES, LANES), LANES)
        for i in range(SIDE):
            act_ref[i, :, cols] = block


def down_kernel(pos_ref, perm_ref, acts, d0, d1, e0, e1, out_ref, res):
    core, x = pos_ref[0], pos_ref[1]
    for own, pair in ((1, (d0, d1)), (0, (e0, e1))):
        total = jnp.zeros((ROWS, 2 * LANES), F32)
        for i in range(SIDE):
            rows = slice(i * BLOCK, (i + 1) * BLOCK)
            both = jnp.concatenate([pair[0][rows, :], pair[1][rows, :]], axis=1)
            total += jnp.dot(acts[i], both, preferred_element_type=F32)
        out = total.astype(BF)
        for k in range(2):
            col = 2 * ((x + k) % 2) + (core if own else 1 - core)
            cols = pl.ds(pl.multiple_of(col * LANES, LANES), LANES)
            res[:, cols] = out[:, k * LANES : (k + 1) * LANES]
    for g in range(CHIPS // GROUP):
        rows = slice(g * SLAB, (g + 1) * SLAB)
        part = jnp.concatenate(
            [res[rows, cb * LANES : (cb + 1) * LANES] for cb in range(SIDE)], axis=0
        )
        n = GROUP * SLAB
        out_ref[g * n : (g + 1) * n, :] = jnp.dot(
            perm_ref[...], part, preferred_element_type=F32
        ).astype(BF)


def call(kernel, out_shape, n_in, flops, nbytes, scratch=(), scalars=True, vmem=24):
    ref = pl.BlockSpec(memory_space=pltpu.VMEM)
    first = [pl.BlockSpec(memory_space=pltpu.SMEM)] if scalars else []
    return pl.pallas_call(
        kernel,
        out_shape=out_shape,
        in_specs=first + [ref] * (n_in - len(first)),
        out_specs=jax.tree.map(lambda _: ref, out_shape),
        scratch_shapes=list(scratch),
        compiler_params=pltpu.CompilerParams(vmem_limit_bytes=vmem * 2**20),
        cost_estimate=pl.CostEstimate(
            flops=flops, bytes_accessed=nbytes, transcendentals=0
        ),
    )


def devices():
    for z in range(CHIPS):
        for c in range(2):
            for y in range(SIDE):
                for x in range(SIDE):
                    yield z, c, y, x


def at(z, c, y, x):
    return (2 * (z % CHIPS) + c) * PLANE + SIDE * y + x


def weight_pairs(k):
    return [
        (at(z, c, y, x), at(z, x % 2, y, 2 * c + (x // 2 + k) % 2))
        for z, c, y, x in devices()
    ]


SIBLING = [(at(z, c, y, x), at(z, 1 - c, y, x)) for z, c, y, x in devices()]
ORDER = [(i * STEP + FIRST) % CHIPS for i in range(CHIPS)]
CORE_GROUPS = [[2 * z + c for z in ORDER] for c in range(2)]
Y_GROUPS = [[SIDE * y + x for y in range(SIDE)] for x in range(SIDE)]
BACK_GROUPS = [
    [at(z, c, y, x) for z in ORDER for x in range(SIDE)]
    for c in range(2)
    for y in range(SIDE)
]
BOTH = ("ep", "tp")


def permute(a, pairs):
    return lax.ppermute(a, BOTH, pairs)


def exchange(a, axes, groups):
    return lax.all_to_all(a, axes, 0, 0, tiled=True, axis_index_groups=groups)


def per_device(tokens, norm_gain, route_ids, route_weights, w_gate, w_up, w_down):
    tp, ep = lax.axis_index("tp"), lax.axis_index("ep")
    x, z, core = tp & 3, ep >> 1, ep & 1
    pos = jnp.stack([core, x, z, tp >> 2]).astype(jnp.int32)
    outgoing = call(
        prep_kernel,
        jax.ShapeDtypeStruct((CHIPS * UNIT, HALF), BF),
        4,
        10**8,
        2 * 10**6,
        vmem=60,
    )(pos, tokens, norm_gain.reshape(1, -1), route_ids.T)
    raw = exchange(outgoing.reshape(CHIPS, UNIT, HALF), "ep", CORE_GROUPS)

    def pick(w, i):
        return lax.dynamic_index_in_dim(w, i, 0, keepdims=False)

    def share(blocks):
        own = [permute(blocks[k], weight_pairs(k)) for k in range(2)]
        return own + [permute(b, SIBLING) for b in own]

    mine = (tp >> 1) & 1
    gu_blocks = share(
        [jnp.stack([pick(w_gate, i), pick(w_up, i)]) for i in (mine, 1 - mine)]
    )
    wd_blocks = share([pick(w_down, i) for i in (mine, 1 - mine)])
    scale = call(
        scale_kernel,
        jax.ShapeDtypeStruct((2, TOK, 4 * ROWS), BF),
        2,
        10**8,
        2 * 10**6,
        scalars=False,
    )(route_ids, route_weights)

    raw = jnp.broadcast_to(
        raw.reshape(1, CHIPS * UNIT, HALF), (SIDE, CHIPS * UNIT, HALF)
    )
    raw = exchange(raw, "tp", Y_GROUPS)
    act = call(
        gate_up_kernel,
        jax.ShapeDtypeStruct((SIDE, ROWS, BLOCK), BF),
        7,
        2 * 10**9,
        6 * 10**6,
        [pltpu.VMEM((ROWS, SIDE * BLOCK), BF)],
    )(pos, jnp.asarray(unpack_matrix(), BF), raw, *gu_blocks)
    acts = exchange(act, "tp", Y_GROUPS)
    result = call(
        down_kernel,
        jax.ShapeDtypeStruct((4 * ROWS, LANES), BF),
        7,
        10**9,
        4 * 10**6,
        [pltpu.VMEM((ROWS, BLOCK), BF)],
    )(pos, jnp.asarray(pack_matrix(), BF), acts, *wd_blocks)
    returned = exchange(
        result.reshape(4 * CHIPS, 3, 4, LANES), BOTH, BACK_GROUPS
    ).reshape(4 * ROWS, LANES)
    return call(
        combine_kernel,
        jax.ShapeDtypeStruct((TOK, LANES), BF),
        2,
        2 * 10**8,
        2 * 10**6,
        scalars=False,
    )(scale, returned)


def solution(mesh):
    return jax.shard_map(
        per_device,
        mesh=mesh,
        in_specs=(
            P("ep", None),
            P(),
            P("ep", None),
            P("ep", None),
            P("ep", None, "tp"),
            P("ep", None, "tp"),
            P("ep", None, "tp"),
        ),
        out_specs=P("ep", "tp"),
        check_vma=False,
    )
```
